32 devices in a mesh: sp: 8 (over z, core), tp: 4 (over y, x).
Axes of the slice: x: 2, y: 2, z: 4, core: 2. Of those that a mesh axis runs over, the one named last changes fastest.
Arguments:
- rec_input: bfloat16 [3072, 3072], P('sp', 'tp'), may hold values from -6 to 6
- gate_input: bfloat16 [3072, 3072], P('sp', 'tp'), may hold values from -6 to 6
- conv_weight: bfloat16 [4, 3072], P(None, 'tp'), may hold values from -3 to 3
- decay_wide: bfloat16 [2, 16, 128, 128], P(None, 'tp'), may hold values from -0.5 to 0.5
- decay_narrow: bfloat16 [2, 16, 64, 64], P(None, 'tp'), may hold values from -0.75 to 0.75
- input_wide: bfloat16 [2, 16, 128, 128], P(None, 'tp'), may hold values from -0.5 to 0.5
- input_narrow: bfloat16 [2, 16, 64, 64], P(None, 'tp'), may hold values from -0.75 to 0.75
- decay_base: float32 [2, 3072], P(None, 'tp'), may hold values from 6.510417e-06 to 8.138021e-05
- decay_extra: float32 [2, 3072, 2, 16], P(None, 'sp', None, 'tp'), may hold values from -1 to 0
- tokens: bfloat16 [3072, 2048], P('sp', 'tp'), may hold values from -16 to 16
- out_weight: bfloat16 [3072, 2048], P(None, 'tp'), may hold values from -0.3125 to 0.3125
- norm_gain: float32 [2048], P('tp'), may hold values from 0.1 to 1.9
- shared_gate: bfloat16 [2048, 2048], P(None, 'tp'), may hold values from -0.125 to 0.125
- shared_up: bfloat16 [2048, 2048], P(None, 'tp'), may hold values from -0.125 to 0.125
- shared_down: bfloat16 [2048, 2048], P(None, 'tp'), may hold values from -0.125 to 0.125
- expert_gate: bfloat16 [8, 2048, 2048], P('sp', None, 'tp'), may hold values from -0.125 to 0.125
- expert_up: bfloat16 [8, 2048, 2048], P('sp', None, 'tp'), may hold values from -0.125 to 0.125
- expert_down: bfloat16 [8, 2048, 2048], P('sp', None, 'tp'), may hold values from -0.125 to 0.125
- routes: int32 [3072, 2], P('sp'), may hold values from 0 to 7, all different within a row; in each aligned block of 384 rows (0 to 383, 384 to 767, ...) at most 144 rows name the same one
- route_weight: float32 [3072, 2], P('sp'), may hold values from 0.2 to 1.5
Outputs:
- layer_out: bfloat16 [3072, 2048], P('sp', 'tp')
The draws below stay inside these ranges and needn't reach their ends.
Inputs may be any that keep to these rules, and one draw needn't show every extreme that they name: `routes`: each row names 2 different experts. The rows of one index of sp name no expert more than 144 times, and in some such block one expert exactly 144 times.
All inputs are finite; a program needn't handle non-finite values.
Results may differ from the reference program's by a relative error of at most 0.0052.
Values may be sent and summed in bfloat16 or wider, within the bound.
A program may use at most 64 MiB of HBM per device.

```python
import math
import jax
import jax.numpy as jnp
import numpy as np
from jax import lax

D = 2048
HEADS = 16
HEAD_WIDE = 128
HEAD_NARROW = 64
CONV = 4
FF = 2048
TOP = 2
TOK_DEV = 384
W = 3072
TOKENS = 3072
EXPERTS = 8
CAP = 144
N_SP = 8


def draw_decay_extra(key, part):
    keys = jax.random.split(key, 5)
    slow_share = 0.5
    slow_heads = (jax.random.uniform(keys[0], (2, 1, 2, HEADS)) < slow_share).astype(jnp.float32)
    quick_decay_rate = jax.random.uniform(keys[1], (2, 1, 2, HEADS), minval=0.02, maxval=0.05)
    block_count = TOKENS // TOK_DEV
    block_factor = jnp.exp(jax.random.uniform(keys[2], (2, block_count, 1, 2, HEADS), minval=0.0, maxval=1.1))
    block_factor = jnp.broadcast_to(block_factor, (2, block_count, TOK_DEV, 2, HEADS)).reshape(2, TOKENS, 2, HEADS)
    slow_rate = block_factor * (0.3 / TOKENS)
    surplus_term = -(slow_heads * slow_rate + (1.0 - slow_heads) * quick_decay_rate)
    target_locations = jax.random.randint(keys[3], (3, 2, 1, 2, HEADS), 0, TOKENS)
    extent_list = jnp.log(jax.random.uniform(keys[4], (3, 2, 1, 2, HEADS), minval=0.5, maxval=0.8))
    token_positions = jnp.arange(TOKENS, dtype=jnp.int32)[None, :, None, None]
    for spike_amount in range(3):
        surplus_term = surplus_term + jnp.where(token_positions == target_locations[spike_amount], extent_list[spike_amount], 0.0)
    return surplus_term.astype(jnp.float32)


def draw_tokens(key, part):
    column = jnp.arange(D, dtype=jnp.float32)[None, :]
    scale = 1.0 + 2.0 * column / D
    base = jnp.clip(jax.random.normal(key, (TOKENS, D)), -5.0, 5.0)
    return (base * scale).astype(jnp.bfloat16)


def steps_of(own_key, shape, cuts, smallest, largest):
    factor_of, own = 1.0, jax.random.fold_in(own_key, 6)
    for axis_at, parts in cuts:
        steps = jnp.exp(jax.random.uniform(jax.random.fold_in(own, axis_at), (parts,), jnp.float32, smallest / len(cuts), largest / len(cuts)))
        factor_of = factor_of * jnp.repeat(steps, shape[axis_at] // parts).reshape([-1 if axis == axis_at else 1 for axis in range(len(shape))])
    return factor_of


def assign_block(own_key, own, number, rows, count, top, bound, lean):
    sequence = jax.random.permutation(own_key, count)
    heavy_load, usual = load_shares(count, rows * top, bound, lean, True), load_shares(count, rows * top, bound, lean, False)
    places = jnp.arange(count)

    def named(tallies, turn):
        used = int((tallies > 0).sum())
        fixed = max(1, used // 4)
        moved = fixed + (places - fixed + turn * (used - fixed)) % max(1, count - fixed)
        return jnp.zeros((count,), jnp.int32).at[sequence[jnp.where(places < fixed, places, moved)]].set(jnp.asarray(tallies, jnp.int32))

    tallies = jnp.where(number % 4 == 0, named(heavy_load, number // 4), named(usual, number - number // 4 - 1))
    mixed = jax.random.permutation(jax.random.fold_in(own, 3), count)
    giver, receiver = mixed[0:count // 2 * 2:2], mixed[1:count // 2 * 2:2]
    slack = jnp.minimum(tallies[giver] - 1, bound - tallies[receiver]) // 2
    slack = jnp.where((giver == sequence[0]) | (receiver == sequence[0]) | (tallies[receiver] == 0), 0, jnp.maximum(slack, 0))
    moved = jax.random.randint(jax.random.fold_in(own, 4), (count // 2,), 0, 1 << 20) % (slack + 1)
    tallies = tallies.at[giver].add(-moved).at[receiver].add(moved)
    labels = jnp.searchsorted(jnp.cumsum(tallies), jnp.arange(rows * top), side="right").astype(jnp.int32)
    grid = labels.reshape(top, rows).T
    grid = grid[jax.random.permutation(jax.random.fold_in(own, 1), rows)]
    turn = jax.random.randint(jax.random.fold_in(own, 2), (rows, 1), 0, top)
    return jnp.take_along_axis(grid, (jnp.arange(top)[None, :] + turn) % top, axis=1)


def load_shares(count, total, most, slope, full):
    loads = [(1 << 20) // math.isqrt(standing ** slope) + 1 for standing in range(1, count + 1)]
    largest = most if full else min(most, max(-(-total // count), total * loads[0] // sum(loads)))
    least = 1 if total - largest >= count - 1 else 0
    given, surplus = [largest] + [least] * (count - 1), total - largest - least * (count - 1)
    while surplus > 0:
        free = [i for i in range(1, count) if given[i] < largest] or [i for i in range(1, count) if given[i] < most]
        whole, remaining = sum([loads[i] for i in free]), surplus
        for i in free:
            more = min(most - given[i], max(1, remaining * loads[i] // whole), surplus)
            given[i] = given[i] + more
            surplus = surplus - more
    return np.array(given)


def bell_draw(own_key, extent, deviation, bound, cuts=(), kind=jnp.bfloat16):
    result = deviation * jax.random.normal(own_key, extent, jnp.float32)
    if cuts:
        result = result * steps_of(own_key, extent, cuts, -0.22, 0.18)
    return jnp.clip(result, -bound, bound).astype(kind)


def setup_inputs(seed: int = 0) -> dict:
    arg_keys = jax.random.split(jax.random.key(seed), 21)
    rec_input = bell_draw(arg_keys[0], (TOKENS, W), 1.0, 6.0, ((0, 8), (1, 4)))
    gate_input = bell_draw(arg_keys[1], (TOKENS, W), 1.0, 6.0, ((0, 8), (1, 4)))
    conv_weight = bell_draw(arg_keys[2], (CONV, W), CONV ** -0.5, 3.0, ((1, 4),))
    decay_wide = bell_draw(arg_keys[3], (2, HEADS, HEAD_WIDE, HEAD_WIDE), HEAD_WIDE ** -0.5, 0.5, ((1, 4),))
    decay_narrow = bell_draw(arg_keys[4], (2, HEADS, HEAD_NARROW, HEAD_NARROW), HEAD_NARROW ** -0.5, 0.75, ((1, 4),))
    input_wide = bell_draw(arg_keys[5], (2, HEADS, HEAD_WIDE, HEAD_WIDE), HEAD_WIDE ** -0.5, 0.5, ((1, 4),))
    input_narrow = bell_draw(arg_keys[6], (2, HEADS, HEAD_NARROW, HEAD_NARROW), HEAD_NARROW ** -0.5, 0.75, ((1, 4),))
    decay_base = jnp.clip(jnp.exp(math.log(8.138021075865254e-05) - 2.5257286 * jax.random.uniform(arg_keys[7], (2, W), jnp.float32) ** steps_of(arg_keys[7], (2, W), ((1, 4),), -0.2, 0.2)), 6.510416824312415e-06, 8.138021075865254e-05)
    decay_extra = draw_decay_extra(jax.random.fold_in(arg_keys[20], 71), 0)
    tokens = draw_tokens(jax.random.fold_in(arg_keys[20], 71), 0)
    out_weight = bell_draw(arg_keys[10], (W, D), (W // 9) ** -0.5, 0.3125, ((1, 4),))
    norm_gain = jnp.clip(1.0 + 0.18 * jax.random.normal(arg_keys[11], (D,), jnp.float32), 0.1, 1.9)
    shared_gate = bell_draw(arg_keys[12], (D, FF), D ** -0.5, 0.125, ((1, 4),))
    shared_up = bell_draw(arg_keys[13], (D, FF), D ** -0.5, 0.125, ((1, 4),))
    shared_down = bell_draw(arg_keys[14], (FF, D), FF ** -0.5, 0.125, ((1, 4),))
    expert_gate = bell_draw(arg_keys[15], (EXPERTS, D, FF), D ** -0.5, 0.125, ((0, 8), (2, 4)))
    expert_up = bell_draw(arg_keys[16], (EXPERTS, D, FF), D ** -0.5, 0.125, ((0, 8), (2, 4)))
    expert_down = bell_draw(arg_keys[17], (EXPERTS, FF, D), FF ** -0.5, 0.125, ((0, 8), (2, 4)))
    routes_keys = jax.random.split(jax.random.fold_in(arg_keys[18], 1), TOKENS // TOK_DEV)
    routes_turns = jax.random.permutation(jax.random.fold_in(arg_keys[18], 3), TOKENS // TOK_DEV)
    routes = jax.vmap(lambda own, number: assign_block(jax.random.fold_in(arg_keys[18], 2), own, number, TOK_DEV, EXPERTS, TOP, CAP, 2))(routes_keys, routes_turns).reshape((TOKENS, TOP))
    route_weight = jnp.clip(0.2 + 1.3 * jax.random.uniform(arg_keys[19], (TOKENS, TOP), jnp.float32) ** steps_of(arg_keys[19], (TOKENS, TOP), ((0, 8),), -0.2, 0.2), 0.2, 1.5)
    return {"rec_input": rec_input, "gate_input": gate_input, "conv_weight": conv_weight, "decay_wide": decay_wide, "decay_narrow": decay_narrow, "input_wide": input_wide, "input_narrow": input_narrow, "decay_base": decay_base, "decay_extra": decay_extra, "tokens": tokens, "out_weight": out_weight, "norm_gain": norm_gain, "shared_gate": shared_gate, "shared_up": shared_up, "shared_down": shared_down, "expert_gate": expert_gate, "expert_up": expert_up, "expert_down": expert_down, "routes": routes, "route_weight": route_weight}


NORM_EPS = 1e-06
RATE_SCALE = 8.0

def link(earlier, latter):
    return (earlier[0] * latter[0], latter[0] * earlier[1] + latter[1])

def run_scan(decays, drives, reverse):
    if reverse:
        decays = jnp.flip(decays, 0)
        drives = jnp.flip(drives, 0)
    cumulative, states = lax.associative_scan(link, (decays, drives), axis=0)
    if reverse:
        states = jnp.flip(states, 0)
    return states

def channels_per_head(per_head):
    row_count = per_head.shape[0]
    head_count = per_head.shape[2]
    wide_part = jnp.broadcast_to(per_head[:, 0, :, None], (row_count, head_count, HEAD_WIDE))
    narrow_part = jnp.broadcast_to(per_head[:, 1, :, None], (row_count, head_count, HEAD_NARROW))
    return jnp.concatenate([wide_part, narrow_part], axis=2).reshape(row_count, -1)

def block_gate(grouped, wide_blocks, narrow_blocks):
    wide_in = grouped[:, :, :HEAD_WIDE]
    narrow_in = grouped[:, :, HEAD_WIDE:]
    wide_out = jnp.einsum('thi,hij->thj', wide_in, wide_blocks.astype(jnp.float32))
    narrow_out = jnp.einsum('thi,hij->thj', narrow_in, narrow_blocks.astype(jnp.float32))
    joined = jnp.concatenate([wide_out, narrow_out], axis=2)
    return jax.nn.sigmoid(joined.reshape(grouped.shape[0], -1))

def reference(rec_input, gate_input, conv_weight, decay_wide, decay_narrow, input_wide, input_narrow, decay_base, decay_extra, tokens, out_weight, norm_gain, shared_gate, shared_up, shared_down, expert_gate, expert_up, expert_down, routes, route_weight):
    row_count = rec_input.shape[0]
    padded = jnp.pad(rec_input.astype(jnp.float32), ((2, 1), (0, 0)))
    conv_sum = padded[0:row_count] * conv_weight[0].astype(jnp.float32)
    for tap_index in range(1, CONV):
        conv_sum = conv_sum + padded[tap_index:tap_index + row_count] * conv_weight[tap_index].astype(jnp.float32)
    conv_out = conv_sum.astype(jnp.bfloat16)
    conv_wide = conv_out.astype(jnp.float32)
    grouped = conv_wide.reshape(row_count, HEADS, HEAD_WIDE + HEAD_NARROW)
    summed = jnp.zeros((row_count, W), jnp.float32)
    for direction in range(2):
        rate = block_gate(grouped, decay_wide[direction], decay_narrow[direction])
        admit = block_gate(grouped, input_wide[direction], input_narrow[direction])
        log_decay = -RATE_SCALE * rate * decay_base[direction][None, :] + channels_per_head(decay_extra[direction])
        drives = jnp.sqrt(-jnp.expm1(2.0 * log_decay)) * admit * conv_wide
        summed = summed + run_scan(jnp.exp(log_decay), drives, direction == 1)
    mixed = (summed * jax.nn.gelu(gate_input.astype(jnp.float32))).astype(jnp.bfloat16)
    resid = tokens.astype(jnp.float32) + jnp.dot(mixed, out_weight, preferred_element_type=jnp.float32)
    scale_row = lax.rsqrt(lax.optimization_barrier(jnp.mean(resid * resid, axis=1, keepdims=True)) + NORM_EPS)
    normed = (resid * scale_row * norm_gain[None, :]).astype(jnp.bfloat16)
    shared_expert_hidden = (jax.nn.silu(jnp.dot(normed, shared_gate, preferred_element_type=jnp.float32)) * jnp.dot(normed, shared_up, preferred_element_type=jnp.float32)).astype(jnp.bfloat16)
    shared_out = jnp.dot(shared_expert_hidden, shared_down, preferred_element_type=jnp.float32)
    most_rows = N_SP * CAP

    def expert_step(routed_sum, inputs):
        gate_weights, up_weights, down_weights, expert_id = inputs
        matches = routes == expert_id
        weight_row = lax.optimization_barrier(jnp.sum(jnp.where(matches, route_weight, 0.0), axis=1))
        selected = jnp.any(matches, axis=1)
        row_index = jnp.nonzero(selected, size=most_rows, fill_value=0)[0].astype(jnp.int32)
        live_count = jnp.sum(selected.astype(jnp.int32))
        is_live = jnp.arange(most_rows, dtype=jnp.int32) < live_count
        picked = normed[row_index]
        hidden = (jax.nn.silu(jnp.dot(picked, gate_weights, preferred_element_type=jnp.float32)) * jnp.dot(picked, up_weights, preferred_element_type=jnp.float32)).astype(jnp.bfloat16)
        expert_out = jnp.dot(hidden, down_weights, preferred_element_type=jnp.float32).astype(jnp.bfloat16).astype(jnp.float32)
        weights = jnp.where(is_live, weight_row[row_index], 0.0)
        routed_sum = routed_sum.at[row_index].add(weights[:, None] * expert_out)
        return (routed_sum, None)
    routed_sum, unused = lax.scan(expert_step, jnp.zeros((row_count, D), jnp.float32), (expert_gate, expert_up, expert_down, jnp.arange(EXPERTS, dtype=jnp.int32)))
    return (resid + shared_out + routed_sum).astype(jnp.bfloat16)
```

```python
import functools

import jax
import jax.numpy as jnp
import numpy as np
from jax import lax
from jax.experimental import pallas as pl
from jax.experimental.pallas import tpu as pltpu
from jax.sharding import PartitionSpec as P

MESH = pl.DeviceIdType.MESH
D = 2048
CONV = 4
NORM_EPS = 1e-06
RATE_SCALE = 8.0
SEG = 8
F32 = jnp.float32
BF16 = jnp.bfloat16
EXACT = lax.Precision.HIGHEST


def rcopy(src, dst, send, recv, **where):
    return pltpu.make_async_remote_copy(
        src_ref=src, dst_ref=dst, send_sem=send, recv_sem=recv, device_id=where, device_id_type=MESH
    )


def greet(n_sp, n_tp):
    sp, tp = lax.axis_index("sp"), lax.axis_index("tp")
    barrier = pltpu.get_barrier_semaphore()
    for k in range(1, n_sp):
        pl.semaphore_signal(
            barrier, inc=1, device_id={"sp": lax.rem(sp + k, n_sp)}, device_id_type=MESH
        )
    for k in range(1, n_tp):
        pl.semaphore_signal(
            barrier, inc=1, device_id={"tp": lax.rem(tp + k, n_tp)}, device_id_type=MESH
        )
    pl.semaphore_wait(barrier, n_sp + n_tp - 2)


def gather_sems(n_tp):
    count = 6 if n_tp == 4 else n_tp
    return [pltpu.SemaphoreType.DMA((count,)), pltpu.SemaphoreType.DMA((count,))]


class Gather:
    def __init__(self, n_tp, slot, send, recv, base=0):
        self.n, self.slot, self.send, self.recv, self.base = n_tp, slot, send, recv, base
        self.t = lax.axis_index("tp")
        if n_tp == 4:
            y, x = self.t // 2, lax.rem(self.t, 2)
            self.xn, self.yn, self.dg = y * 2 + 1 - x, (1 - y) * 2 + x, 3 - self.t

    def piece(self, owner, half, sem, to):
        ref = self.slot(owner, half)
        s = self.base + sem
        return rcopy(ref, ref, self.send.at[s], self.recv.at[s], tp=to)

    def start(self):
        if self.n == 4:
            self.piece(self.t, 0, 0, self.xn).start()
            self.piece(self.t, 1, 3, self.yn).start()
            self.piece(self.t, 1, 1, self.xn).start()
            self.piece(self.t, 0, 2, self.yn).start()
        else:
            for k in range(1, self.n):
                to = lax.rem(self.t + k, self.n)
                self.piece(self.t, None, k, to).start()

    def forward(self):
        if self.n == 4:
            self.piece(self.xn, 0, 0, self.xn).wait_recv()
            self.piece(self.xn, 0, 4, self.yn).start()
            self.piece(self.yn, 1, 3, self.yn).wait_recv()
            self.piece(self.yn, 1, 5, self.xn).start()

    def arrivals(self):
        if self.n == 4:
            self.piece(self.xn, 1, 1, self.xn).wait_recv()
            yield self.xn
            self.piece(self.yn, 0, 2, self.yn).wait_recv()
            yield self.yn
            self.piece(self.dg, 0, 4, self.yn).wait_recv()
            self.piece(self.dg, 1, 5, self.xn).wait_recv()
            yield self.dg
        else:
            for k in range(1, self.n):
                owner = lax.rem(self.t - k + self.n, self.n)
                self.piece(owner, None, k, owner).wait_recv()
                yield owner

    def drain(self):
        if self.n == 4:
            for s, half, owner in (
                (0, 0, self.t), (1, 1, self.t), (2, 0, self.t), (3, 1, self.t),
                (4, 0, self.xn), (5, 1, self.yn),
            ):
                self.piece(owner, half, s, self.xn).wait_send()
        else:
            for k in range(1, self.n):
                to = lax.rem(self.t + k, self.n)
                self.piece(self.t, None, k, to).wait_send()


def minus_expm1(y):
    series = 1.0 + y * (1 / 7.0)
    for d in (6.0, 5.0, 4.0, 3.0, 2.0):
        series = 1.0 + y * (1 / d) * series
    return jnp.where(y > -0.3, -y * series, 1.0 - jnp.exp(y))


def front_kernel(
    n_sp, n_tp,
    rec, gate, convw, wblk, base, extra, spread, perm, permt, tokens, outw, gain,
    resid, whole, normed,
    halo, cperm, gperm, av, bv, msg, totals, mixedp, mixed, squares, sqown,
    hsend, hrecv, tsend, trecv, gsend, grecv, ssend, srecv, nsend, nrecv,
):
    rows, chan = rec.shape
    groups, gw = wblk.shape[1], wblk.shape[2]
    cols = tokens.shape[1]
    seglen = rows // SEG
    sp, tp = lax.axis_index("sp"), lax.axis_index("tp")
    greet(n_sp, n_tp)
    up, down = lax.rem(sp + 1, n_sp), lax.rem(sp + n_sp - 1, n_sp)
    low = rcopy(rec.at[pl.ds(rows - 16, 16)], halo.at[0], hsend.at[0], hrecv.at[0], sp=up)
    high = rcopy(rec.at[pl.ds(0, 16)], halo.at[1], hsend.at[1], hrecv.at[1], sp=down)
    low.start()
    high.start()

    gperm[...] = jnp.dot(permt[...], gate[...], preferred_element_type=F32).astype(BF16)
    low.wait()
    high.wait()
    x = rec[...].astype(F32)
    lo = jnp.where(sp > 0, halo[0].astype(F32), 0.0)
    hi = jnp.where(sp < n_sp - 1, halo[1].astype(F32), 0.0)
    padded = jnp.concatenate([lo[14:16], x, hi[0:1]], axis=0)
    conv = padded[0:rows] * convw[0:1, :]
    for j in range(1, CONV):
        conv = conv + padded[j : j + rows] * convw[j : j + 1, :]
    cperm[...] = jnp.dot(
        permt[...], conv.astype(BF16), preferred_element_type=F32
    ).astype(BF16)

    step = 64

    @pl.loop(0, rows // step)
    def _(r):
        at = pl.ds(pl.multiple_of(r * step, step), step)
        for d in range(2):
            ex = jnp.dot(extra[d, at, :], spread[...], precision=EXACT, preferred_element_type=F32)
            for g in range(groups):
                lanes = slice(g * gw, (g + 1) * gw)
                c = cperm[at, lanes]
                rate = jax.nn.sigmoid(jnp.dot(c, wblk[2 * d, g], preferred_element_type=F32))
                admit = jax.nn.sigmoid(jnp.dot(c, wblk[2 * d + 1, g], preferred_element_type=F32))
                ld = -RATE_SCALE * rate * base[d : d + 1, lanes] + ex[:, lanes]
                bv[d, at, lanes] = jnp.sqrt(minus_expm1(2.0 * ld)) * admit * c.astype(F32)
                av[d, at, lanes] = jnp.exp(ld)

    one = jnp.ones((SEG, chan), F32)
    zero = jnp.zeros((SEG, chan), F32)

    def advance(i, carry):
        out = []
        for d in range(2):
            at = pl.ds(pl.multiple_of((i if d == 0 else seglen - 1 - i) * SEG, SEG), SEG)
            a, b = av[d, at, :], bv[d, at, :]
            cum = carry[2 * d] * a
            state = a * carry[2 * d + 1] + b
            av[d, at, :] = cum
            bv[d, at, :] = state
            out += [cum, state]
        return tuple(out)

    ends = lax.fori_loop(0, seglen, advance, (one, zero, one, zero))

    def run(d, entering):
        order = range(SEG) if d == 0 else range(SEG - 1, -1, -1)
        inside = [None] * SEG
        c = entering
        for s in order:
            inside[s] = c
            c = ends[2 * d][s : s + 1] * c + ends[2 * d + 1][s : s + 1]
        return jnp.concatenate(inside, axis=0), c

    for d in range(2):
        prod = ends[2 * d][0:1]
        for s in range(1, SEG):
            prod = prod * ends[2 * d][s : s + 1]
        msg[2 * d : 2 * d + 1, :] = prod
        msg[2 * d + 1 : 2 * d + 2, :] = run(d, jnp.zeros((1, chan), F32))[1]
    msg[4:8, :] = jnp.zeros((4, chan), F32)
    sent = []
    for k in range(1, n_sp):
        to = lax.rem(sp + k, n_sp)
        c = rcopy(msg, totals.at[k], tsend.at[k], trecv.at[k], sp=to)
        c.start()
        sent.append(c)
    for c in sent:
        c.wait()
    carries = []
    zrow = jnp.zeros((1, chan), F32)
    c0, c1 = zrow, zrow
    for k in range(n_sp - 1, 0, -1):
        t = totals[k]
        c0 = jnp.where(k <= sp, t[0:1] * c0 + t[1:2], c0)
    for k in range(1, n_sp):
        t = totals[k]
        c1 = jnp.where(k > sp, t[2:3] * c1 + t[3:4], c1)
    for d, c in ((0, c0), (1, c1)):
        inside = run(d, c)[0]
        carries.append(jnp.concatenate([inside, inside], axis=0))

    @pl.loop(0, rows // 16)
    def _(r):
        at = pl.ds(pl.multiple_of(r * 16, 16), 16)
        total = bv[0, at, :] + av[0, at, :] * carries[0]
        total = total + (bv[1, at, :] + av[1, at, :] * carries[1])
        mixedp[at, :] = (total * jax.nn.gelu(gperm[at, :].astype(F32))).astype(BF16)

    mixed[tp] = jnp.dot(perm[...], mixedp[...], preferred_element_type=F32).astype(BF16)

    half = rows // 2

    def mixed_slot(owner, part):
        return mixed.at[owner] if part is None else mixed.at[owner, pl.ds(part * half, half)]

    g = Gather(n_tp, mixed_slot, gsend, grecv)
    g.start()
    resid[...] = tokens[...].astype(F32)

    def project(owner):
        @pl.loop(0, rows // 128)
        def _(r):
            at = pl.ds(pl.multiple_of(r * 128, 128), 128)
            resid[at, :] += jnp.dot(mixed[owner, at, :], outw[owner], preferred_element_type=F32)

    project(tp)
    g.forward()
    for owner in g.arrivals():
        project(owner)

    r2 = resid[...] * resid[...]
    sqown[...] = lax.dot_general(
        jnp.ones((8, cols), F32), r2, (((1,), (1,)), ((), ())),
        precision=EXACT, preferred_element_type=F32,
    )
    sent = []
    for k in range(1, n_tp):
        c = rcopy(sqown, squares.at[k], ssend.at[k], srecv.at[k], tp=lax.rem(tp + k, n_tp))
        c.start()
        sent.append(c)
    total = sqown[...]
    for k, c in enumerate(sent):
        c.wait()
        total = total + squares[k + 1]
    scale = lax.rsqrt(total / D + NORM_EPS)
    scale = lax.dot_general(
        scale, jnp.full((8, 128), 0.125, F32), (((0,), (0,)), ((), ())),
        precision=EXACT, preferred_element_type=F32,
    )[:, 0:1]
    normed[...] = (resid[...] * scale * gain[...]).astype(BF16)
    mine = pl.ds(pl.multiple_of(tp * cols, 128), cols)
    whole[:, mine] = normed[...]

    def normed_slot(owner, part):
        lanes = pl.ds(pl.multiple_of(owner * cols, 128), cols)
        at = pl.ds(0, rows) if part is None else pl.ds(part * half, half)
        return whole.at[at, lanes]

    h = Gather(n_tp, normed_slot, nsend, nrecv)
    h.start()
    g.drain()
    h.forward()
    for owner in h.arrivals():
        pass
    h.drain()


def front(n_sp, n_tp, rec, gate, conv_weight, dw, dn, iw, inn, base, extra, tokens, outw, gain):
    rows, chan = rec.shape
    heads, wide, narrow = dw.shape[1], dw.shape[2], dn.shape[2]
    cols = tokens.shape[1]
    per = 2 if heads % 2 == 0 else 1
    hw = wide + narrow
    gw = per * hw
    blocks = []
    for d in range(2):
        for w, n in ((dw, dn), (iw, inn)):
            w = w[d].reshape(heads // per, per, wide, wide)
            n = n[d].reshape(heads // per, per, narrow, narrow)
            block = 0
            for p in range(per):
                a = p * hw
                z = ((0, 0), (a, gw - a - wide), (a, gw - a - wide))
                block = block + jnp.pad(w[:, p], z)
                a += wide
                z = ((0, 0), (a, gw - a - narrow), (a, gw - a - narrow))
                block = block + jnp.pad(n[:, p], z)
            blocks.append(block)
    wblk = jnp.stack(blocks)
    seglen = rows // SEG
    ex = extra.reshape(2, SEG, seglen, 2 * heads).swapaxes(1, 2).reshape(2, rows, 2 * heads)
    c = np.arange(chan)
    which = (c % hw >= wide) * heads + c // hw
    spread = jnp.asarray((which[None, :] == np.arange(2 * heads)[:, None]).astype(np.float32))
    r = lax.broadcasted_iota(jnp.int32, (rows, rows), 0)
    q = lax.broadcasted_iota(jnp.int32, (rows, rows), 1)
    permt = ((r % SEG) * seglen + r // SEG == q).astype(BF16)
    perm = ((q % SEG) * seglen + q // SEG == r).astype(BF16)
    vm = pl.BlockSpec(memory_space=pltpu.VMEM)
    dma = pltpu.SemaphoreType.DMA
    return pl.pallas_call(
        functools.partial(front_kernel, n_sp, n_tp),
        name="front",
        out_shape=(
            jax.ShapeDtypeStruct((rows, cols), F32),
            jax.ShapeDtypeStruct((rows, n_tp * cols), BF16),
            jax.ShapeDtypeStruct((rows, cols), BF16),
        ),
        in_specs=[vm] * 12,
        out_specs=(vm, vm, vm),
        scratch_shapes=[
            pltpu.VMEM((2, 16, chan), BF16),
            pltpu.VMEM((rows, chan), BF16),
            pltpu.VMEM((rows, chan), BF16),
            pltpu.VMEM((2, rows, chan), F32),
            pltpu.VMEM((2, rows, chan), F32),
            pltpu.VMEM((8, chan), F32),
            pltpu.VMEM((n_sp, 8, chan), F32),
            pltpu.VMEM((rows, chan), BF16),
            pltpu.VMEM((n_tp, rows, chan), BF16),
            pltpu.VMEM((n_tp, 8, rows), F32),
            pltpu.VMEM((8, rows), F32),
            dma((2,)), dma((2,)), dma((n_sp,)), dma((n_sp,)),
            *gather_sems(n_tp), dma((n_tp,)), dma((n_tp,)), *gather_sems(n_tp),
        ],
        compiler_params=pltpu.CompilerParams(
            collective_id=0, has_side_effects=True, vmem_limit_bytes=60 * 1024 * 1024
        ),
    )(
        rec, gate, conv_weight.astype(F32), wblk, base, ex, spread, perm, permt, tokens,
        outw.reshape(n_tp, chan, cols), gain.reshape(1, cols),
    )


def shards(
    rec_input,
    gate_input,
    conv_weight,
    decay_wide,
    decay_narrow,
    input_wide,
    input_narrow,
    decay_base,
    decay_extra,
    tokens,
    out_weight,
    norm_gain,
    shared_gate,
    shared_up,
    shared_down,
    expert_gate,
    expert_up,
    expert_down,
    routes,
    route_weight,
):
    seq_rows = rec_input.shape[0]
    columns = out_weight.shape[1]
    resid, whole_rows, normed = front(
        lax.axis_size("sp"), lax.axis_size("tp"), rec_input, gate_input, conv_weight,
        decay_wide, decay_narrow, input_wide, input_narrow, decay_base, decay_extra,
        tokens, out_weight, norm_gain,
    )
    width_all = whole_rows.shape[1]
    top_count = routes.shape[1]
    expert_count = lax.axis_size("sp")
    capacity = 3 * seq_rows * top_count // (2 * expert_count)
    flat_route = routes.reshape(-1)
    onehot = (flat_route[:, None] == jnp.arange(expert_count, dtype=jnp.int32)[None, :]).astype(
        jnp.int32
    )
    before = jnp.cumsum(onehot, axis=0) - onehot
    slot_ids = jnp.sum(before * onehot, axis=1)
    placing = flat_route * capacity + slot_ids
    owner_rows = jnp.arange(seq_rows * top_count, dtype=jnp.int32) // top_count
    slot_table = (
        jnp.full((expert_count * capacity,), seq_rows, jnp.int32).at[placing].set(owner_rows)
    )
    padded_cols = jnp.concatenate([normed, jnp.zeros((1, columns), jnp.bfloat16)], axis=0)
    outgoing = padded_cols[slot_table].reshape(expert_count, capacity, columns)
    arrived = lax.all_to_all(outgoing, "sp", split_axis=0, concat_axis=0, tiled=True)
    expert_rows = lax.all_gather(arrived, "tp", axis=2, tiled=True).reshape(-1, width_all)
    routed_hidden = (
        jax.nn.silu(jnp.dot(expert_rows, expert_gate[0], preferred_element_type=jnp.float32))
        * jnp.dot(expert_rows, expert_up[0], preferred_element_type=jnp.float32)
    ).astype(jnp.bfloat16)
    shared_expert_hidden = (
        jax.nn.silu(jnp.dot(whole_rows, shared_gate, preferred_element_type=jnp.float32))
        * jnp.dot(whole_rows, shared_up, preferred_element_type=jnp.float32)
    ).astype(jnp.bfloat16)
    down_local = expert_down[0]
    routed_out = jnp.dot(
        lax.all_gather(routed_hidden, "tp", axis=1, tiled=True),
        down_local,
        preferred_element_type=jnp.float32,
    )
    shared_out = jnp.dot(
        lax.all_gather(shared_expert_hidden, "tp", axis=1, tiled=True),
        shared_down,
        preferred_element_type=jnp.float32,
    )
    sending = routed_out.astype(jnp.bfloat16).reshape(expert_count, capacity, columns)
    returned = lax.all_to_all(sending, "sp", split_axis=0, concat_axis=0, tiled=True)
    picked = (
        returned.reshape(-1, columns)[placing]
        .reshape(seq_rows, top_count, columns)
        .astype(jnp.float32)
    )
    combined = jnp.sum(route_weight[:, :, None] * picked, axis=1)
    return (resid + shared_out + combined).astype(jnp.bfloat16)


def solution(mesh):
    placed = (
        P("sp", "tp"),
        P("sp", "tp"),
        P(None, "tp"),
        P(None, "tp", None, None),
        P(None, "tp", None, None),
        P(None, "tp", None, None),
        P(None, "tp", None, None),
        P(None, "tp"),
        P(None, "sp", None, "tp"),
        P("sp", "tp"),
        P(None, "tp"),
        P("tp"),
        P(None, "tp"),
        P(None, "tp"),
        P(None, "tp"),
        P("sp", None, "tp"),
        P("sp", None, "tp"),
        P("sp", None, "tp"),
        P("sp", None),
        P("sp", None),
    )
    return jax.shard_map(
        shards, mesh=mesh, in_specs=placed, out_specs=P("sp", "tp"), check_vma=False
    )
```

```python
import functools

import jax
import jax.numpy as jnp
import numpy as np
from jax import lax
from jax.experimental import pallas as pl
from jax.experimental.pallas import tpu as pltpu
from jax.sharding import PartitionSpec as P

MESH = pl.DeviceIdType.MESH
D = 2048
CONV = 4
NORM_EPS = 1e-06
RATE_SCALE = 8.0
SEG = 8
F32 = jnp.float32
BF16 = jnp.bfloat16
EXACT = lax.Precision.HIGHEST


def rcopy(src, dst, send, recv, **where):
    return pltpu.make_async_remote_copy(
        src_ref=src, dst_ref=dst, send_sem=send, recv_sem=recv, device_id=where, device_id_type=MESH
    )


def greet(n_sp, n_tp):
    sp, tp = lax.axis_index("sp"), lax.axis_index("tp")
    barrier = pltpu.get_barrier_semaphore()
    for k in range(1, n_sp):
        pl.semaphore_signal(
            barrier, inc=1, device_id={"sp": lax.rem(sp + k, n_sp)}, device_id_type=MESH
        )
    for k in range(1, n_tp):
        pl.semaphore_signal(
            barrier, inc=1, device_id={"tp": lax.rem(tp + k, n_tp)}, device_id_type=MESH
        )
    pl.semaphore_wait(barrier, n_sp + n_tp - 2)


def gather_sems(n_tp):
    count = 6 if n_tp == 4 else n_tp
    return [pltpu.SemaphoreType.DMA((count,)), pltpu.SemaphoreType.DMA((count,))]


class Gather:
    def __init__(self, n_tp, slot, send, recv, base=0):
        self.n, self.slot, self.send, self.recv, self.base = n_tp, slot, send, recv, base
        self.t = lax.axis_index("tp")
        if n_tp == 4:
            y, x = self.t // 2, lax.rem(self.t, 2)
            self.xn, self.yn, self.dg = y * 2 + 1 - x, (1 - y) * 2 + x, 3 - self.t

    def piece(self, owner, half, sem, to):
        ref = self.slot(owner, half)
        s = self.base + sem
        return rcopy(ref, ref, self.send.at[s], self.recv.at[s], tp=to)

    def start(self):
        if self.n == 4:
            self.piece(self.t, 0, 0, self.xn).start()
            self.piece(self.t, 1, 3, self.yn).start()
            self.piece(self.t, 1, 1, self.xn).start()
            self.piece(self.t, 0, 2, self.yn).start()
        else:
            for k in range(1, self.n):
                to = lax.rem(self.t + k, self.n)
                self.piece(self.t, None, k, to).start()

    def forward(self):
        if self.n == 4:
            self.piece(self.xn, 0, 0, self.xn).wait_recv()
            self.piece(self.xn, 0, 4, self.yn).start()
            self.piece(self.yn, 1, 3, self.yn).wait_recv()
            self.piece(self.yn, 1, 5, self.xn).start()

    def arrivals(self):
        if self.n == 4:
            self.piece(self.xn, 1, 1, self.xn).wait_recv()
            yield self.xn
            self.piece(self.yn, 0, 2, self.yn).wait_recv()
            yield self.yn
            self.piece(self.dg, 0, 4, self.yn).wait_recv()
            self.piece(self.dg, 1, 5, self.xn).wait_recv()
            yield self.dg
        else:
            for k in range(1, self.n):
                owner = lax.rem(self.t - k + self.n, self.n)
                self.piece(owner, None, k, owner).wait_recv()
                yield owner

    def drain(self):
        if self.n == 4:
            for s, half, owner in (
                (0, 0, self.t), (1, 1, self.t), (2, 0, self.t), (3, 1, self.t),
                (4, 0, self.xn), (5, 1, self.yn),
            ):
                self.piece(owner, half, s, self.xn).wait_send()
        else:
            for k in range(1, self.n):
                to = lax.rem(self.t + k, self.n)
                self.piece(self.t, None, k, to).wait_send()


def minus_expm1(y):
    series = 1.0 + y * (1 / 7.0)
    for d in (6.0, 5.0, 4.0, 3.0, 2.0):
        series = 1.0 + y * (1 / d) * series
    return jnp.where(y > -0.3, -y * series, 1.0 - jnp.exp(y))


def front_kernel(
    n_sp, n_tp,
    rec, gate, convw, wblk, base, extra, spread, perm, permt, tokens, outw, gain,
    resid, whole, normed,
    halo, cperm, gperm, av, bv, msg, totals, mixedp, mixed, squares, sqown,
    hsend, hrecv, tsend, trecv, gsend, grecv, ssend, srecv, nsend, nrecv,
):
    rows, chan = rec.shape
    groups, gw = wblk.shape[1], wblk.shape[2]
    cols = tokens.shape[1]
    seglen = rows // SEG
    sp, tp = lax.axis_index("sp"), lax.axis_index("tp")
    greet(n_sp, n_tp)
    up, down = lax.rem(sp + 1, n_sp), lax.rem(sp + n_sp - 1, n_sp)
    low = rcopy(rec.at[pl.ds(rows - 16, 16)], halo.at[0], hsend.at[0], hrecv.at[0], sp=up)
    high = rcopy(rec.at[pl.ds(0, 16)], halo.at[1], hsend.at[1], hrecv.at[1], sp=down)
    low.start()
    high.start()

    gperm[...] = jnp.dot(permt[...], gate[...], preferred_element_type=F32).astype(BF16)
    low.wait()
    high.wait()
    x = rec[...].astype(F32)
    lo = jnp.where(sp > 0, halo[0].astype(F32), 0.0)
    hi = jnp.where(sp < n_sp - 1, halo[1].astype(F32), 0.0)
    padded = jnp.concatenate([lo[14:16], x, hi[0:1]], axis=0)
    conv = padded[0:rows] * convw[0:1, :]
    for j in range(1, CONV):
        conv = conv + padded[j : j + rows] * convw[j : j + 1, :]
    cperm[...] = jnp.dot(
        permt[...], conv.astype(BF16), preferred_element_type=F32
    ).astype(BF16)

    step = 64

    @pl.loop(0, rows // step)
    def _(r):
        at = pl.ds(pl.multiple_of(r * step, step), step)
        for d in range(2):
            ex = jnp.dot(extra[d, at, :], spread[...], precision=EXACT, preferred_element_type=F32)
            for g in range(groups):
                lanes = slice(g * gw, (g + 1) * gw)
                c = cperm[at, lanes]
                rate = jax.nn.sigmoid(jnp.dot(c, wblk[2 * d, g], preferred_element_type=F32))
                admit = jax.nn.sigmoid(jnp.dot(c, wblk[2 * d + 1, g], preferred_element_type=F32))
                ld = -RATE_SCALE * rate * base[d : d + 1, lanes] + ex[:, lanes]
                bv[d, at, lanes] = jnp.sqrt(minus_expm1(2.0 * ld)) * admit * c.astype(F32)
                av[d, at, lanes] = jnp.exp(ld)

    one = jnp.ones((SEG, chan), F32)
    zero = jnp.zeros((SEG, chan), F32)

    def advance(i, carry):
        out = []
        for d in range(2):
            at = pl.ds(pl.multiple_of((i if d == 0 else seglen - 1 - i) * SEG, SEG), SEG)
            a, b = av[d, at, :], bv[d, at, :]
            cum = carry[2 * d] * a
            state = a * carry[2 * d + 1] + b
            av[d, at, :] = cum
            bv[d, at, :] = state
            out += [cum, state]
        return tuple(out)

    ends = lax.fori_loop(0, seglen, advance, (one, zero, one, zero))

    def run(d, entering):
        order = range(SEG) if d == 0 else range(SEG - 1, -1, -1)
        inside = [None] * SEG
        c = entering
        for s in order:
            inside[s] = c
            c = ends[2 * d][s : s + 1] * c + ends[2 * d + 1][s : s + 1]
        return jnp.concatenate(inside, axis=0), c

    for d in range(2):
        prod = ends[2 * d][0:1]
        for s in range(1, SEG):
            prod = prod * ends[2 * d][s : s + 1]
        msg[2 * d : 2 * d + 1, :] = prod
        msg[2 * d + 1 : 2 * d + 2, :] = run(d, jnp.zeros((1, chan), F32))[1]
    msg[4:8, :] = jnp.zeros((4, chan), F32)
    sent = []
    for k in range(1, n_sp):
        to = lax.rem(sp + k, n_sp)
        c = rcopy(msg, totals.at[k], tsend.at[k], trecv.at[k], sp=to)
        c.start()
        sent.append(c)
    for c in sent:
        c.wait()
    carries = []
    zrow = jnp.zeros((1, chan), F32)
    c0, c1 = zrow, zrow
    for k in range(n_sp - 1, 0, -1):
        t = totals[k]
        c0 = jnp.where(k <= sp, t[0:1] * c0 + t[1:2], c0)
    for k in range(1, n_sp):
        t = totals[k]
        c1 = jnp.where(k > sp, t[2:3] * c1 + t[3:4], c1)
    for d, c in ((0, c0), (1, c1)):
        inside = run(d, c)[0]
        carries.append(jnp.concatenate([inside, inside], axis=0))

    @pl.loop(0, rows // 16)
    def _(r):
        at = pl.ds(pl.multiple_of(r * 16, 16), 16)
        total = bv[0, at, :] + av[0, at, :] * carries[0]
        total = total + (bv[1, at, :] + av[1, at, :] * carries[1])
        mixedp[at, :] = (total * jax.nn.gelu(gperm[at, :].astype(F32))).astype(BF16)

    mixed[tp] = jnp.dot(perm[...], mixedp[...], preferred_element_type=F32).astype(BF16)

    half = rows // 2

    def mixed_slot(owner, part):
        return mixed.at[owner] if part is None else mixed.at[owner, pl.ds(part * half, half)]

    g = Gather(n_tp, mixed_slot, gsend, grecv)
    g.start()
    resid[...] = tokens[...].astype(F32)

    def project(owner):
        @pl.loop(0, rows // 128)
        def _(r):
            at = pl.ds(pl.multiple_of(r * 128, 128), 128)
            resid[at, :] += jnp.dot(mixed[owner, at, :], outw[owner], preferred_element_type=F32)

    project(tp)
    g.forward()
    for owner in g.arrivals():
        project(owner)

    r2 = resid[...] * resid[...]
    sqown[...] = lax.dot_general(
        jnp.ones((8, cols), F32), r2, (((1,), (1,)), ((), ())),
        precision=EXACT, preferred_element_type=F32,
    )
    sent = []
    for k in range(1, n_tp):
        c = rcopy(sqown, squares.at[k], ssend.at[k], srecv.at[k], tp=lax.rem(tp + k, n_tp))
        c.start()
        sent.append(c)
    total = sqown[...]
    for k, c in enumerate(sent):
        c.wait()
        total = total + squares[k + 1]
    scale = lax.rsqrt(total / D + NORM_EPS)
    scale = lax.dot_general(
        scale, jnp.full((8, 128), 0.125, F32), (((0,), (0,)), ((), ())),
        precision=EXACT, preferred_element_type=F32,
    )[:, 0:1]
    normed[...] = (resid[...] * scale * gain[...]).astype(BF16)
    mine = pl.ds(pl.multiple_of(tp * cols, 128), cols)
    whole[:, mine] = normed[...]

    def normed_slot(owner, part):
        lanes = pl.ds(pl.multiple_of(owner * cols, 128), cols)
        at = pl.ds(0, rows) if part is None else pl.ds(part * half, half)
        return whole.at[at, lanes]

    h = Gather(n_tp, normed_slot, nsend, nrecv)
    h.start()
    g.drain()
    h.forward()
    for owner in h.arrivals():
        pass
    h.drain()


def front(n_sp, n_tp, rec, gate, conv_weight, dw, dn, iw, inn, base, extra, tokens, outw, gain):
    rows, chan = rec.shape
    heads, wide, narrow = dw.shape[1], dw.shape[2], dn.shape[2]
    cols = tokens.shape[1]
    per = 2 if heads % 2 == 0 else 1
    hw = wide + narrow
    gw = per * hw
    blocks = []
    for d in range(2):
        for w, n in ((dw, dn), (iw, inn)):
            w = w[d].reshape(heads // per, per, wide, wide)
            n = n[d].reshape(heads // per, per, narrow, narrow)
            block = 0
            for p in range(per):
                a = p * hw
                z = ((0, 0), (a, gw - a - wide), (a, gw - a - wide))
                block = block + jnp.pad(w[:, p], z)
                a += wide
                z = ((0, 0), (a, gw - a - narrow), (a, gw - a - narrow))
                block = block + jnp.pad(n[:, p], z)
            blocks.append(block)
    wblk = jnp.stack(blocks)
    seglen = rows // SEG
    ex = extra.reshape(2, SEG, seglen, 2 * heads).swapaxes(1, 2).reshape(2, rows, 2 * heads)
    c = np.arange(chan)
    which = (c % hw >= wide) * heads + c // hw
    spread = jnp.asarray((which[None, :] == np.arange(2 * heads)[:, None]).astype(np.float32))
    r = lax.broadcasted_iota(jnp.int32, (rows, rows), 0)
    q = lax.broadcasted_iota(jnp.int32, (rows, rows), 1)
    permt = ((r % SEG) * seglen + r // SEG == q).astype(BF16)
    perm = ((q % SEG) * seglen + q // SEG == r).astype(BF16)
    vm = pl.BlockSpec(memory_space=pltpu.VMEM)
    dma = pltpu.SemaphoreType.DMA
    return pl.pallas_call(
        functools.partial(front_kernel, n_sp, n_tp),
        name="front",
        out_shape=(
            jax.ShapeDtypeStruct((rows, cols), F32),
            jax.ShapeDtypeStruct((rows, n_tp * cols), BF16),
            jax.ShapeDtypeStruct((rows, cols), BF16),
        ),
        in_specs=[vm] * 12,
        out_specs=(vm, vm, vm),
        scratch_shapes=[
            pltpu.VMEM((2, 16, chan), BF16),
            pltpu.VMEM((rows, chan), BF16),
            pltpu.VMEM((rows, chan), BF16),
            pltpu.VMEM((2, rows, chan), F32),
            pltpu.VMEM((2, rows, chan), F32),
            pltpu.VMEM((8, chan), F32),
            pltpu.VMEM((n_sp, 8, chan), F32),
            pltpu.VMEM((rows, chan), BF16),
            pltpu.VMEM((n_tp, rows, chan), BF16),
            pltpu.VMEM((n_tp, 8, rows), F32),
            pltpu.VMEM((8, rows), F32),
            dma((2,)), dma((2,)), dma((n_sp,)), dma((n_sp,)),
            *gather_sems(n_tp), dma((n_tp,)), dma((n_tp,)), *gather_sems(n_tp),
        ],
        compiler_params=pltpu.CompilerParams(
            collective_id=0, has_side_effects=True, vmem_limit_bytes=60 * 1024 * 1024
        ),
    )(
        rec, gate, conv_weight.astype(F32), wblk, base, ex, spread, perm, permt, tokens,
        outw.reshape(n_tp, chan, cols), gain.reshape(1, cols),
    )


def experts_kernel(
    n_sp, n_tp, cap,
    prow, pcol, weight, resid, whole, normed, hbm_sg, hbm_su, hbm_eg, hbm_eu, hbm_ed, hbm_sd,
    out,
    sg, su, eg, eu, ed, sd, outgoing, rows_in, hidden, answer, returned, shid, acc,
    wsem, dsend, drecv, asend, arecv, bsend, brecv, csend, crecv, rsend, rrecv,
):
    rows, cols = normed.shape
    ff = eg.shape[1]
    sp, tp = lax.axis_index("sp"), lax.axis_index("tp")
    count = 6 if n_tp == 4 else n_tp
    loads = []
    for i, (a, b) in enumerate(
        ((hbm_sg, sg), (hbm_su, su), (hbm_eg, eg), (hbm_eu, eu), (hbm_ed, ed), (hbm_sd, sd))
    ):
        c = pltpu.make_async_copy(a, b, wsem.at[i])
        c.start()
        loads.append(c)
    greet(n_sp, n_tp)

    slot = lax.broadcasted_iota(jnp.int32, (cap, rows), 0)
    mine = pl.ds(pl.multiple_of(tp * cols, 128), cols)
    fmine = pl.ds(pl.multiple_of(tp * ff, 128), ff)

    def dispatch(k):
        to = lax.rem(sp + k, n_sp)
        return rcopy(
            outgoing.at[to], rows_in.at[sp, :, mine], dsend.at[k], drecv.at[k], sp=to
        )

    def landed(k):
        src = lax.rem(sp - k + n_sp, n_sp)
        return rcopy(
            outgoing.at[src], rows_in.at[src, :, mine], dsend.at[k], drecv.at[k], sp=src
        )

    def reply(k):
        src = lax.rem(sp - k + n_sp, n_sp)
        return rcopy(answer.at[src], returned.at[sp], rsend.at[k], rrecv.at[k], sp=src)

    def replied(k):
        e = lax.rem(sp + k, n_sp)
        return rcopy(answer.at[e], returned.at[e], rsend.at[k], rrecv.at[k], sp=e)

    @pl.loop(0, n_sp)
    def _(k):
        e = lax.rem(sp + k, n_sp)
        hit = (prow[0:1, :] - e * cap == slot) | (prow[1:2, :] - e * cap == slot)
        picked = jnp.dot(
            hit.astype(F32).astype(BF16), normed[...], preferred_element_type=F32
        ).astype(BF16)

        @pl.when(k == 0)
        def _():
            rows_in[sp, :, mine] = picked

        @pl.when(k > 0)
        def _():
            outgoing[e] = picked
            dispatch(k).start()

    def gather(buffer, width, send, recv, k):
        src = lax.rem(sp - k + n_sp, n_sp)

        def place(owner, part):
            if part is None:
                return buffer.at[src, :, pl.ds(pl.multiple_of(owner * width, 128), width)]
            half = width // 2
            first = pl.multiple_of(owner * width + part * half, 128)
            return buffer.at[src, :, pl.ds(first, half)]

        return Gather(n_tp, place, send, recv, base=k * count)

    def rows_gather(k):
        return gather(rows_in, cols, asend, arecv, k)

    def hidden_gather(k):
        return gather(hidden, ff, bsend, brecv, k)

    def shared_place(owner, part):
        if part is None:
            return shid.at[:, pl.ds(pl.multiple_of(owner * ff, 128), ff)]
        half = ff // 2
        first = pl.multiple_of(owner * ff + part * half, 128)
        return shid.at[:, pl.ds(first, half)]

    shared = Gather(n_tp, shared_place, csend, crecv)
    rows_gather(0).start()
    loads[0].wait()
    loads[1].wait()

    @pl.loop(0, rows // 128)
    def _(r):
        at = pl.ds(pl.multiple_of(r * 128, 128), 128)
        x = whole[at, :]
        g = jnp.dot(x, sg[...], preferred_element_type=F32)
        u = jnp.dot(x, su[...], preferred_element_type=F32)
        shid[at, fmine] = (jax.nn.silu(g) * u).astype(BF16)

    for c in loads[2:5]:
        c.wait()

    @pl.loop(0, n_sp + 4)
    def _(step):
        @pl.when((step > 0) & (step < n_sp))
        def _():
            landed(step).wait_recv()
            rows_gather(step).start()

        @pl.when((step >= 1) & (step < n_sp + 1))
        def _():
            rows_gather(step - 1).forward()

        @pl.when((step >= 2) & (step < n_sp + 2))
        def _():
            k = step - 2
            src = lax.rem(sp - k + n_sp, n_sp)
            for _ in rows_gather(k).arrivals():
                pass
            x = rows_in[src]
            g = jnp.dot(x, eg[...], preferred_element_type=F32)
            u = jnp.dot(x, eu[...], preferred_element_type=F32)
            hidden[src, :, fmine] = (jax.nn.silu(g) * u).astype(BF16)
            hidden_gather(k).start()

        @pl.when(step == n_sp + 1)
        def _():
            shared.start()

        @pl.when((step >= 3) & (step < n_sp + 3))
        def _():
            hidden_gather(step - 3).forward()

        @pl.when(step >= 4)
        def _():
            k = step - 4
            src = lax.rem(sp - k + n_sp, n_sp)
            for _ in hidden_gather(k).arrivals():
                pass
            y = jnp.dot(hidden[src], ed[...], preferred_element_type=F32).astype(BF16)

            @pl.when(k == 0)
            def _():
                returned[sp] = y

            @pl.when(k > 0)
            def _():
                answer[src] = y
                reply(k).start()

    shared.forward()
    loads[5].wait()
    for _ in shared.arrivals():
        pass

    @pl.loop(0, rows // 128)
    def _(r):
        at = pl.ds(pl.multiple_of(r * 128, 128), 128)
        acc[at, :] = resid[at, :] + jnp.dot(shid[at, :], sd[...], preferred_element_type=F32)

    @pl.loop(0, n_sp)
    def _(k):
        e = lax.rem(sp + k, n_sp)

        @pl.when(k > 0)
        def _():
            replied(k).wait_recv()

        lane = lax.broadcasted_iota(jnp.int32, (128, cap), 1)

        @pl.loop(0, rows // 128)
        def _(r):
            at = pl.ds(pl.multiple_of(r * 128, 128), 128)
            p0 = pcol[at, 0:1] - e * cap
            p1 = pcol[at, 1:2] - e * cap
            w = jnp.where((p0 >= 0) & (p0 < cap), weight[at, 0:1], 0.0) + jnp.where(
                (p1 >= 0) & (p1 < cap), weight[at, 1:2], 0.0
            )
            hit = ((p0 == lane) | (p1 == lane)).astype(F32).astype(BF16)
            acc[at, :] += w * jnp.dot(hit, returned[e], preferred_element_type=F32)

    out[...] = acc[...].astype(BF16)
    shared.drain()

    @pl.loop(0, n_sp)
    def _(k):
        rows_gather(k).drain()
        hidden_gather(k).drain()

        @pl.when(k > 0)
        def _():
            dispatch(k).wait_send()
            reply(k).wait_send()


def experts(n_sp, n_tp, cap, placing, route_weight, resid, whole, normed, weights):
    rows, cols = normed.shape
    ff = weights[0].shape[1]
    vm = pl.BlockSpec(memory_space=pltpu.VMEM)
    hbm = pl.BlockSpec(memory_space=pl.ANY)
    dma = pltpu.SemaphoreType.DMA
    count = 6 if n_tp == 4 else n_tp
    return pl.pallas_call(
        functools.partial(experts_kernel, n_sp, n_tp, cap),
        name="experts",
        out_shape=jax.ShapeDtypeStruct((rows, cols), BF16),
        in_specs=[vm] * 6 + [hbm] * 6,
        out_specs=vm,
        scratch_shapes=[pltpu.VMEM(w.shape, BF16) for w in weights] + [
            pltpu.VMEM((n_sp, cap, cols), BF16),
            pltpu.VMEM((n_sp, cap, n_tp * cols), BF16),
            pltpu.VMEM((n_sp, cap, n_tp * ff), BF16),
            pltpu.VMEM((n_sp, cap, cols), BF16),
            pltpu.VMEM((n_sp, cap, cols), BF16),
            pltpu.VMEM((rows, n_tp * ff), BF16),
            pltpu.VMEM((rows, cols), F32),
            dma((6,)), dma((n_sp,)), dma((n_sp,)),
            dma((n_sp * count,)), dma((n_sp * count,)),
            dma((n_sp * count,)), dma((n_sp * count,)),
            *gather_sems(n_tp), dma((n_sp,)), dma((n_sp,)),
        ],
        compiler_params=pltpu.CompilerParams(
            collective_id=1, has_side_effects=True, vmem_limit_bytes=60 * 1024 * 1024
        ),
    )(placing.T, placing, route_weight, resid, whole, normed, *weights)


def shards(
    rec_input,
    gate_input,
    conv_weight,
    decay_wide,
    decay_narrow,
    input_wide,
    input_narrow,
    decay_base,
    decay_extra,
    tokens,
    out_weight,
    norm_gain,
    shared_gate,
    shared_up,
    shared_down,
    expert_gate,
    expert_up,
    expert_down,
    routes,
    route_weight,
):
    seq_rows = rec_input.shape[0]
    columns = out_weight.shape[1]
    resid, whole_rows, normed = front(
        lax.axis_size("sp"), lax.axis_size("tp"), rec_input, gate_input, conv_weight,
        decay_wide, decay_narrow, input_wide, input_narrow, decay_base, decay_extra,
        tokens, out_weight, norm_gain,
    )
    top_count = routes.shape[1]
    expert_count = lax.axis_size("sp")
    capacity = 3 * seq_rows * top_count // (2 * expert_count)
    flat_route = routes.reshape(-1)
    onehot = (flat_route[:, None] == jnp.arange(expert_count, dtype=jnp.int32)[None, :]).astype(
        jnp.int32
    )
    before = jnp.cumsum(onehot, axis=0) - onehot
    slot_ids = jnp.sum(before * onehot, axis=1)
    placing = (flat_route * capacity + slot_ids).reshape(seq_rows, top_count)
    return experts(
        expert_count, lax.axis_size("tp"), capacity, placing, route_weight, resid, whole_rows, normed,
        (shared_gate, shared_up, expert_gate[0], expert_up[0], expert_down[0], shared_down),
    )


def solution(mesh):
    placed = (
        P("sp", "tp"),
        P("sp", "tp"),
        P(None, "tp"),
        P(None, "tp", None, None),
        P(None, "tp", None, None),
        P(None, "tp", None, None),
        P(None, "tp", None, None),
        P(None, "tp"),
        P(None, "sp", None, "tp"),
        P("sp", "tp"),
        P(None, "tp"),
        P("tp"),
        P(None, "tp"),
        P(None, "tp"),
        P(None, "tp"),
        P("sp", None, "tp"),
        P("sp", None, "tp"),
        P("sp", None, "tp"),
        P("sp", None),
        P("sp", None),
    )
    return jax.shard_map(
        shards, mesh=mesh, in_specs=placed, out_specs=P("sp", "tp"), check_vma=False
    )
```

```python
import functools

import jax
import jax.numpy as jnp
import numpy as np
from jax import lax
from jax.experimental import pallas as pl
from jax.experimental.pallas import tpu as pltpu
from jax.sharding import PartitionSpec as P

MESH = pl.DeviceIdType.MESH
D = 2048
CONV = 4
NORM_EPS = 1e-06
RATE_SCALE = 8.0
SEG = 8
F32 = jnp.float32
BF16 = jnp.bfloat16
EXACT = lax.Precision.HIGHEST


def rcopy(src, dst, send, recv, **where):
    return pltpu.make_async_remote_copy(
        src_ref=src, dst_ref=dst, send_sem=send, recv_sem=recv, device_id=where, device_id_type=MESH
    )


def greet(n_sp, n_tp):
    sp, tp = lax.axis_index("sp"), lax.axis_index("tp")
    barrier = pltpu.get_barrier_semaphore()
    for k in range(1, n_sp):
        pl.semaphore_signal(
            barrier, inc=1, device_id={"sp": lax.rem(sp + k, n_sp)}, device_id_type=MESH
        )
    for k in range(1, n_tp):
        pl.semaphore_signal(
            barrier, inc=1, device_id={"tp": lax.rem(tp + k, n_tp)}, device_id_type=MESH
        )
    pl.semaphore_wait(barrier, n_sp + n_tp - 2)


def gather_sems(n_tp):
    count = 6 if n_tp == 4 else n_tp
    return [pltpu.SemaphoreType.DMA((count,)), pltpu.SemaphoreType.DMA((count,))]


class Gather:
    def __init__(self, n_tp, slot, send, recv, base=0):
        self.n, self.slot, self.send, self.recv, self.base = n_tp, slot, send, recv, base
        self.t = lax.axis_index("tp")
        if n_tp == 4:
            y, x = self.t // 2, lax.rem(self.t, 2)
            self.xn, self.yn, self.dg = y * 2 + 1 - x, (1 - y) * 2 + x, 3 - self.t

    def piece(self, owner, half, sem, to):
        ref = self.slot(owner, half)
        s = self.base + sem
        return rcopy(ref, ref, self.send.at[s], self.recv.at[s], tp=to)

    def start(self):
        if self.n == 4:
            self.piece(self.t, 0, 0, self.xn).start()
            self.piece(self.t, 1, 3, self.yn).start()
            self.piece(self.t, 1, 1, self.xn).start()
            self.piece(self.t, 0, 2, self.yn).start()
        else:
            for k in range(1, self.n):
                to = lax.rem(self.t + k, self.n)
                self.piece(self.t, None, k, to).start()

    def forward(self):
        if self.n == 4:
            self.piece(self.xn, 0, 0, self.xn).wait_recv()
            self.piece(self.xn, 0, 4, self.yn).start()
            self.piece(self.yn, 1, 3, self.yn).wait_recv()
            self.piece(self.yn, 1, 5, self.xn).start()

    def arrivals(self):
        if self.n == 4:
            self.piece(self.xn, 1, 1, self.xn).wait_recv()
            yield self.xn
            self.piece(self.yn, 0, 2, self.yn).wait_recv()
            yield self.yn
            self.piece(self.dg, 0, 4, self.yn).wait_recv()
            self.piece(self.dg, 1, 5, self.xn).wait_recv()
            yield self.dg
        else:
            for k in range(1, self.n):
                owner = lax.rem(self.t - k + self.n, self.n)
                self.piece(owner, None, k, owner).wait_recv()
                yield owner

    def drain(self):
        if self.n == 4:
            for s, half, owner in (
                (0, 0, self.t), (1, 1, self.t), (2, 0, self.t), (3, 1, self.t),
                (4, 0, self.xn), (5, 1, self.yn),
            ):
                self.piece(owner, half, s, self.xn).wait_send()
        else:
            for k in range(1, self.n):
                to = lax.rem(self.t + k, self.n)
                self.piece(self.t, None, k, to).wait_send()


def minus_expm1(y):
    series = 1.0 + y * (1 / 7.0)
    for d in (6.0, 5.0, 4.0, 3.0, 2.0):
        series = 1.0 + y * (1 / d) * series
    return jnp.where(y > -0.3, -y * series, 1.0 - jnp.exp(y))


def front_kernel(
    n_sp, n_tp,
    rec, gate, convw, wblk, base, extra, spread, perm, permt, tokens, hbm_outw, gain,
    resid, whole, normed,
    halo, cperm, gperm, av, bv, msg, totals, mixedp, mixed, squares, sqown,
    hsend, hrecv, tsend, trecv, gsend, grecv, ssend, srecv, nsend, nrecv, outw, wsem,
):
    rows, chan = rec.shape
    groups, gw = wblk.shape[1], wblk.shape[2]
    cols = tokens.shape[1]
    seglen = rows // SEG
    sp, tp = lax.axis_index("sp"), lax.axis_index("tp")
    load = pltpu.make_async_copy(hbm_outw, outw, wsem.at[0])
    load.start()
    greet(n_sp, n_tp)
    up, down = lax.rem(sp + 1, n_sp), lax.rem(sp + n_sp - 1, n_sp)
    low = rcopy(rec.at[pl.ds(rows - 16, 16)], halo.at[0], hsend.at[0], hrecv.at[0], sp=up)
    high = rcopy(rec.at[pl.ds(0, 16)], halo.at[1], hsend.at[1], hrecv.at[1], sp=down)
    low.start()
    high.start()

    gperm[...] = jnp.dot(permt[...], gate[...], preferred_element_type=F32).astype(BF16)
    low.wait()
    high.wait()
    x = rec[...].astype(F32)
    lo = jnp.where(sp > 0, halo[0].astype(F32), 0.0)
    hi = jnp.where(sp < n_sp - 1, halo[1].astype(F32), 0.0)
    padded = jnp.concatenate([lo[14:16], x, hi[0:1]], axis=0)
    conv = padded[0:rows] * convw[0:1, :]
    for j in range(1, CONV):
        conv = conv + padded[j : j + rows] * convw[j : j + 1, :]
    cperm[...] = jnp.dot(
        permt[...], conv.astype(BF16), preferred_element_type=F32
    ).astype(BF16)

    step = 64

    @pl.loop(0, rows // step)
    def _(r):
        at = pl.ds(pl.multiple_of(r * step, step), step)
        for d in range(2):
            ex = jnp.dot(extra[d, at, :], spread[...], precision=EXACT, preferred_element_type=F32)
            for g in range(groups):
                lanes = slice(g * gw, (g + 1) * gw)
                c = cperm[at, lanes]
                rate = jax.nn.sigmoid(jnp.dot(c, wblk[2 * d, g], preferred_element_type=F32))
                admit = jax.nn.sigmoid(jnp.dot(c, wblk[2 * d + 1, g], preferred_element_type=F32))
                ld = -RATE_SCALE * rate * base[d : d + 1, lanes] + ex[:, lanes]
                bv[d, at, lanes] = jnp.sqrt(minus_expm1(2.0 * ld)) * admit * c.astype(F32)
                av[d, at, lanes] = jnp.exp(ld)

    one = jnp.ones((SEG, chan), F32)
    zero = jnp.zeros((SEG, chan), F32)

    def advance(i, carry):
        out = []
        for d in range(2):
            at = pl.ds(pl.multiple_of((i if d == 0 else seglen - 1 - i) * SEG, SEG), SEG)
            a, b = av[d, at, :], bv[d, at, :]
            cum = carry[2 * d] * a
            state = a * carry[2 * d + 1] + b
            av[d, at, :] = cum
            bv[d, at, :] = state
            out += [cum, state]
        return tuple(out)

    ends = lax.fori_loop(0, seglen, advance, (one, zero, one, zero))

    def run(d, entering):
        order = range(SEG) if d == 0 else range(SEG - 1, -1, -1)
        inside = [None] * SEG
        c = entering
        for s in order:
            inside[s] = c
            c = ends[2 * d][s : s + 1] * c + ends[2 * d + 1][s : s + 1]
        return jnp.concatenate(inside, axis=0), c

    for d in range(2):
        prod = ends[2 * d][0:1]
        for s in range(1, SEG):
            prod = prod * ends[2 * d][s : s + 1]
        msg[2 * d : 2 * d + 1, :] = prod
        msg[2 * d + 1 : 2 * d + 2, :] = run(d, jnp.zeros((1, chan), F32))[1]
    msg[4:8, :] = jnp.zeros((4, chan), F32)
    sent = []
    for k in range(1, n_sp):
        to = lax.rem(sp + k, n_sp)
        c = rcopy(msg, totals.at[k], tsend.at[k], trecv.at[k], sp=to)
        c.start()
        sent.append(c)
    for c in sent:
        c.wait()
    carries = []
    zrow = jnp.zeros((1, chan), F32)
    c0, c1 = zrow, zrow
    for k in range(n_sp - 1, 0, -1):
        t = totals[k]
        c0 = jnp.where(k <= sp, t[0:1] * c0 + t[1:2], c0)
    for k in range(1, n_sp):
        t = totals[k]
        c1 = jnp.where(k > sp, t[2:3] * c1 + t[3:4], c1)
    for d, c in ((0, c0), (1, c1)):
        inside = run(d, c)[0]
        carries.append(jnp.concatenate([inside, inside], axis=0))

    @pl.loop(0, rows // 16)
    def _(r):
        at = pl.ds(pl.multiple_of(r * 16, 16), 16)
        total = bv[0, at, :] + av[0, at, :] * carries[0]
        total = total + (bv[1, at, :] + av[1, at, :] * carries[1])
        mixedp[at, :] = (total * jax.nn.gelu(gperm[at, :].astype(F32))).astype(BF16)

    mixed[tp] = jnp.dot(perm[...], mixedp[...], preferred_element_type=F32).astype(BF16)

    half = rows // 2

    def mixed_slot(owner, part):
        return mixed.at[owner] if part is None else mixed.at[owner, pl.ds(part * half, half)]

    g = Gather(n_tp, mixed_slot, gsend, grecv)
    g.start()
    resid[...] = tokens[...].astype(F32)

    def project(owner):
        @pl.loop(0, rows // 128)
        def _(r):
            at = pl.ds(pl.multiple_of(r * 128, 128), 128)
            resid[at, :] += jnp.dot(mixed[owner, at, :], outw[owner], preferred_element_type=F32)

    load.wait()
    project(tp)
    g.forward()
    for owner in g.arrivals():
        project(owner)

    r2 = resid[...] * resid[...]
    sqown[...] = lax.dot_general(
        jnp.ones((8, cols), F32), r2, (((1,), (1,)), ((), ())),
        precision=EXACT, preferred_element_type=F32,
    )
    sent = []
    for k in range(1, n_tp):
        c = rcopy(sqown, squares.at[k], ssend.at[k], srecv.at[k], tp=lax.rem(tp + k, n_tp))
        c.start()
        sent.append(c)
    total = sqown[...]
    for k, c in enumerate(sent):
        c.wait()
        total = total + squares[k + 1]
    scale = lax.rsqrt(total / D + NORM_EPS)
    scale = lax.dot_general(
        scale, jnp.full((8, 128), 0.125, F32), (((0,), (0,)), ((), ())),
        precision=EXACT, preferred_element_type=F32,
    )[:, 0:1]
    normed[...] = (resid[...] * scale * gain[...]).astype(BF16)
    mine = pl.ds(pl.multiple_of(tp * cols, 128), cols)
    whole[:, mine] = normed[...]

    def normed_slot(owner, part):
        lanes = pl.ds(pl.multiple_of(owner * cols, 128), cols)
        at = pl.ds(0, rows) if part is None else pl.ds(part * half, half)
        return whole.at[at, lanes]

    h = Gather(n_tp, normed_slot, nsend, nrecv)
    h.start()
    g.drain()
    h.forward()
    for owner in h.arrivals():
        pass
    h.drain()


def front(n_sp, n_tp, rec, gate, conv_weight, dw, dn, iw, inn, base, extra, tokens, outw, gain):
    rows, chan = rec.shape
    heads, wide, narrow = dw.shape[1], dw.shape[2], dn.shape[2]
    cols = tokens.shape[1]
    per = 2 if heads % 2 == 0 else 1
    hw = wide + narrow
    gw = per * hw
    blocks = []
    for d in range(2):
        for w, n in ((dw, dn), (iw, inn)):
            w = w[d].reshape(heads // per, per, wide, wide)
            n = n[d].reshape(heads // per, per, narrow, narrow)
            block = 0
            for p in range(per):
                a = p * hw
                z = ((0, 0), (a, gw - a - wide), (a, gw - a - wide))
                block = block + jnp.pad(w[:, p], z)
                a += wide
                z = ((0, 0), (a, gw - a - narrow), (a, gw - a - narrow))
                block = block + jnp.pad(n[:, p], z)
            blocks.append(block)
    wblk = jnp.stack(blocks)
    seglen = rows // SEG
    ex = extra.reshape(2, SEG, seglen, 2 * heads).swapaxes(1, 2).reshape(2, rows, 2 * heads)
    c = np.arange(chan)
    which = (c % hw >= wide) * heads + c // hw
    spread = jnp.asarray((which[None, :] == np.arange(2 * heads)[:, None]).astype(np.float32))
    r = lax.broadcasted_iota(jnp.int32, (rows, rows), 0)
    q = lax.broadcasted_iota(jnp.int32, (rows, rows), 1)
    permt = ((r % SEG) * seglen + r // SEG == q).astype(BF16)
    perm = ((q % SEG) * seglen + q // SEG == r).astype(BF16)
    vm = pl.BlockSpec(memory_space=pltpu.VMEM)
    dma = pltpu.SemaphoreType.DMA
    return pl.pallas_call(
        functools.partial(front_kernel, n_sp, n_tp),
        name="front",
        out_shape=(
            jax.ShapeDtypeStruct((rows, cols), F32),
            jax.ShapeDtypeStruct((rows, n_tp * cols), BF16),
            jax.ShapeDtypeStruct((rows, cols), BF16),
        ),
        in_specs=[vm] * 10 + [pl.BlockSpec(memory_space=pl.ANY), vm],
        out_specs=(vm, vm, vm),
        scratch_shapes=[
            pltpu.VMEM((2, 16, chan), BF16),
            pltpu.VMEM((rows, chan), BF16),
            pltpu.VMEM((rows, chan), BF16),
            pltpu.VMEM((2, rows, chan), F32),
            pltpu.VMEM((2, rows, chan), F32),
            pltpu.VMEM((8, chan), F32),
            pltpu.VMEM((n_sp, 8, chan), F32),
            pltpu.VMEM((rows, chan), BF16),
            pltpu.VMEM((n_tp, rows, chan), BF16),
            pltpu.VMEM((n_tp, 8, rows), F32),
            pltpu.VMEM((8, rows), F32),
            dma((2,)), dma((2,)), dma((n_sp,)), dma((n_sp,)),
            *gather_sems(n_tp), dma((n_tp,)), dma((n_tp,)), *gather_sems(n_tp),
            pltpu.VMEM((n_tp, chan, cols), BF16), dma((1,)),
        ],
        compiler_params=pltpu.CompilerParams(
            collective_id=0, has_side_effects=True, vmem_limit_bytes=60 * 1024 * 1024
        ),
    )(
        rec, gate, conv_weight.astype(F32), wblk, base, ex, spread, perm, permt, tokens,
        outw.reshape(n_tp, chan, cols), gain.reshape(1, cols),
    )


def experts_kernel(
    n_sp, n_tp, cap,
    prow, pcol, weight, resid, whole, normed, hbm_sg, hbm_su, hbm_eg, hbm_eu, hbm_ed, hbm_sd,
    out,
    sg, su, eg, eu, ed, sd, outgoing, rows_in, hidden, answer, returned, shid, acc,
    wsem, dsend, drecv, asend, arecv, bsend, brecv, csend, crecv, rsend, rrecv,
):
    rows, cols = normed.shape
    ff = eg.shape[1]
    sp, tp = lax.axis_index("sp"), lax.axis_index("tp")
    count = 6 if n_tp == 4 else n_tp
    loads = []
    for i, (a, b) in enumerate(
        ((hbm_sg, sg), (hbm_su, su), (hbm_eg, eg), (hbm_eu, eu), (hbm_ed, ed), (hbm_sd, sd))
    ):
        c = pltpu.make_async_copy(a, b, wsem.at[i])
        c.start()
        loads.append(c)
    greet(n_sp, n_tp)

    slot = lax.broadcasted_iota(jnp.int32, (cap, rows), 0)
    mine = pl.ds(pl.multiple_of(tp * cols, 128), cols)
    fmine = pl.ds(pl.multiple_of(tp * ff, 128), ff)

    def dispatch(k):
        to = lax.rem(sp + k, n_sp)
        return rcopy(
            outgoing.at[to], rows_in.at[sp, :, mine], dsend.at[k], drecv.at[k], sp=to
        )

    def landed(k):
        src = lax.rem(sp - k + n_sp, n_sp)
        return rcopy(
            outgoing.at[src], rows_in.at[src, :, mine], dsend.at[k], drecv.at[k], sp=src
        )

    def reply(k):
        src = lax.rem(sp - k + n_sp, n_sp)
        return rcopy(answer.at[src], returned.at[sp], rsend.at[k], rrecv.at[k], sp=src)

    def replied(k):
        e = lax.rem(sp + k, n_sp)
        return rcopy(answer.at[e], returned.at[e], rsend.at[k], rrecv.at[k], sp=e)

    @pl.loop(0, n_sp)
    def _(k):
        e = lax.rem(sp + k, n_sp)
        hit = (prow[0:1, :] - e * cap == slot) | (prow[1:2, :] - e * cap == slot)
        picked = jnp.dot(
            hit.astype(F32).astype(BF16), normed[...], preferred_element_type=F32
        ).astype(BF16)

        @pl.when(k == 0)
        def _():
            rows_in[sp, :, mine] = picked

        @pl.when(k > 0)
        def _():
            outgoing[e] = picked
            dispatch(k).start()

    def gather(buffer, width, send, recv, k):
        src = lax.rem(sp - k + n_sp, n_sp)

        def place(owner, part):
            if part is None:
                return buffer.at[src, :, pl.ds(pl.multiple_of(owner * width, 128), width)]
            half = width // 2
            first = pl.multiple_of(owner * width + part * half, 128)
            return buffer.at[src, :, pl.ds(first, half)]

        return Gather(n_tp, place, send, recv, base=k * count)

    def rows_gather(k):
        return gather(rows_in, cols, asend, arecv, k)

    def hidden_gather(k):
        return gather(hidden, ff, bsend, brecv, k)

    def shared_place(owner, part):
        if part is None:
            return shid.at[:, pl.ds(pl.multiple_of(owner * ff, 128), ff)]
        half = ff // 2
        first = pl.multiple_of(owner * ff + part * half, 128)
        return shid.at[:, pl.ds(first, half)]

    shared = Gather(n_tp, shared_place, csend, crecv)
    rows_gather(0).start()
    loads[0].wait()
    loads[1].wait()

    @pl.loop(0, rows // 128)
    def _(r):
        at = pl.ds(pl.multiple_of(r * 128, 128), 128)
        x = whole[at, :]
        g = jnp.dot(x, sg[...], preferred_element_type=F32)
        u = jnp.dot(x, su[...], preferred_element_type=F32)
        shid[at, fmine] = (jax.nn.silu(g) * u).astype(BF16)

    shared.start()
    for c in loads[2:5]:
        c.wait()

    def combine(k):
        e = lax.rem(sp + k, n_sp)

        @pl.when(k > 0)
        def _():
            replied(k).wait_recv()

        lane = lax.broadcasted_iota(jnp.int32, (128, cap), 1)

        @pl.loop(0, rows // 128)
        def _(r):
            at = pl.ds(pl.multiple_of(r * 128, 128), 128)
            p0 = pcol[at, 0:1] - e * cap
            p1 = pcol[at, 1:2] - e * cap
            w = jnp.where((p0 >= 0) & (p0 < cap), weight[at, 0:1], 0.0) + jnp.where(
                (p1 >= 0) & (p1 < cap), weight[at, 1:2], 0.0
            )
            hit = ((p0 == lane) | (p1 == lane)).astype(F32).astype(BF16)
            acc[at, :] += w * jnp.dot(hit, returned[e], preferred_element_type=F32)

    @pl.loop(0, n_sp + 4)
    def _(step):
        @pl.when((step > 0) & (step < n_sp))
        def _():
            landed(step).wait_recv()
            rows_gather(step).start()

        @pl.when((step >= 1) & (step < n_sp + 1))
        def _():
            rows_gather(step - 1).forward()

        @pl.when((step >= 2) & (step < n_sp + 2))
        def _():
            k = step - 2
            src = lax.rem(sp - k + n_sp, n_sp)
            for _ in rows_gather(k).arrivals():
                pass
            x = rows_in[src]
            g = jnp.dot(x, eg[...], preferred_element_type=F32)
            u = jnp.dot(x, eu[...], preferred_element_type=F32)
            hidden[src, :, fmine] = (jax.nn.silu(g) * u).astype(BF16)
            hidden_gather(k).start()

        @pl.when(step == 1)
        def _():
            shared.forward()

        @pl.when(step == 4)
        def _():
            loads[5].wait()
            for _ in shared.arrivals():
                pass

            @pl.loop(0, rows // 128)
            def _(r):
                at = pl.ds(pl.multiple_of(r * 128, 128), 128)
                acc[at, :] = resid[at, :] + jnp.dot(
                    shid[at, :], sd[...], preferred_element_type=F32
                )

        @pl.when(step >= 6)
        def _():
            combine(step - 6)

        @pl.when((step >= 3) & (step < n_sp + 3))
        def _():
            hidden_gather(step - 3).forward()

        @pl.when(step >= 4)
        def _():
            k = step - 4
            src = lax.rem(sp - k + n_sp, n_sp)
            for _ in hidden_gather(k).arrivals():
                pass
            y = jnp.dot(hidden[src], ed[...], preferred_element_type=F32).astype(BF16)

            @pl.when(k == 0)
            def _():
                returned[sp] = y

            @pl.when(k > 0)
            def _():
                answer[src] = y
                reply(k).start()

    @pl.loop(n_sp - 2, n_sp)
    def _(k):
        combine(k)

    out[...] = acc[...].astype(BF16)
    shared.drain()

    @pl.loop(0, n_sp)
    def _(k):
        rows_gather(k).drain()
        hidden_gather(k).drain()

        @pl.when(k > 0)
        def _():
            dispatch(k).wait_send()
            reply(k).wait_send()


def experts(n_sp, n_tp, cap, placing, route_weight, resid, whole, normed, weights):
    rows, cols = normed.shape
    ff = weights[0].shape[1]
    vm = pl.BlockSpec(memory_space=pltpu.VMEM)
    hbm = pl.BlockSpec(memory_space=pl.ANY)
    dma = pltpu.SemaphoreType.DMA
    count = 6 if n_tp == 4 else n_tp
    return pl.pallas_call(
        functools.partial(experts_kernel, n_sp, n_tp, cap),
        name="experts",
        out_shape=jax.ShapeDtypeStruct((rows, cols), BF16),
        in_specs=[vm] * 6 + [hbm] * 6,
        out_specs=vm,
        scratch_shapes=[pltpu.VMEM(w.shape, BF16) for w in weights] + [
            pltpu.VMEM((n_sp, cap, cols), BF16),
            pltpu.VMEM((n_sp, cap, n_tp * cols), BF16),
            pltpu.VMEM((n_sp, cap, n_tp * ff), BF16),
            pltpu.VMEM((n_sp, cap, cols), BF16),
            pltpu.VMEM((n_sp, cap, cols), BF16),
            pltpu.VMEM((rows, n_tp * ff), BF16),
            pltpu.VMEM((rows, cols), F32),
            dma((6,)), dma((n_sp,)), dma((n_sp,)),
            dma((n_sp * count,)), dma((n_sp * count,)),
            dma((n_sp * count,)), dma((n_sp * count,)),
            *gather_sems(n_tp), dma((n_sp,)), dma((n_sp,)),
        ],
        compiler_params=pltpu.CompilerParams(
            collective_id=1, has_side_effects=True, vmem_limit_bytes=60 * 1024 * 1024
        ),
    )(placing.T, placing, route_weight, resid, whole, normed, *weights)


def shards(
    rec_input,
    gate_input,
    conv_weight,
    decay_wide,
    decay_narrow,
    input_wide,
    input_narrow,
    decay_base,
    decay_extra,
    tokens,
    out_weight,
    norm_gain,
    shared_gate,
    shared_up,
    shared_down,
    expert_gate,
    expert_up,
    expert_down,
    routes,
    route_weight,
):
    seq_rows = rec_input.shape[0]
    columns = out_weight.shape[1]
    resid, whole_rows, normed = front(
        lax.axis_size("sp"), lax.axis_size("tp"), rec_input, gate_input, conv_weight,
        decay_wide, decay_narrow, input_wide, input_narrow, decay_base, decay_extra,
        tokens, out_weight, norm_gain,
    )
    top_count = routes.shape[1]
    expert_count = lax.axis_size("sp")
    capacity = 3 * seq_rows * top_count // (2 * expert_count)
    flat_route = routes.reshape(-1)
    onehot = (flat_route[:, None] == jnp.arange(expert_count, dtype=jnp.int32)[None, :]).astype(
        jnp.int32
    )
    before = jnp.cumsum(onehot, axis=0) - onehot
    slot_ids = jnp.sum(before * onehot, axis=1)
    placing = (flat_route * capacity + slot_ids).reshape(seq_rows, top_count)
    return experts(
        expert_count, lax.axis_size("tp"), capacity, placing, route_weight, resid, whole_rows, normed,
        (shared_gate, shared_up, expert_gate[0], expert_up[0], expert_down[0], shared_down),
    )


def solution(mesh):
    placed = (
        P("sp", "tp"),
        P("sp", "tp"),
        P(None, "tp"),
        P(None, "tp", None, None),
        P(None, "tp", None, None),
        P(None, "tp", None, None),
        P(None, "tp", None, None),
        P(None, "tp"),
        P(None, "sp", None, "tp"),
        P("sp", "tp"),
        P(None, "tp"),
        P("tp"),
        P(None, "tp"),
        P(None, "tp"),
        P(None, "tp"),
        P("sp", None, "tp"),
        P("sp", None, "tp"),
        P("sp", None, "tp"),
        P("sp", None),
        P("sp", None),
    )
    return jax.shard_map(
        shards, mesh=mesh, in_specs=placed, out_specs=P("sp", "tp"), check_vma=False
    )
```
